32 devices in a mesh: grp: 2 (over y), fs: 4 (over z), tp: 4 (over x, core).
Axes of the slice: x: 2, y: 2, z: 4, core: 2. Of those that a mesh axis runs over, the one named last changes fastest.
Arguments:
- tokens: bfloat16 [4096, 2048], P(('grp', 'fs', 'tp')), parts along dimension 0, may hold values from -12 to 12
- norm_gain: float32 [2048], replicated, may hold values from 0.1 to 1.9
- w_in: bfloat16 [2048, 8192], P('fs', 'tp'), may hold values from -0.125 to 0.125
- w_out: bfloat16 [8192, 2048], P('tp', 'fs'), may hold values from -0.0625 to 0.0625
Outputs:
- mixed: bfloat16 [4096, 2048], P(('grp', 'fs', 'tp')), parts along dimension 0
The draws below stay inside these ranges and needn't reach their ends.
There are 2 independent parts, one for each index of `grp`. The reference program is written for one: setup_inputs(seed, part) draws one part's arguments, and reference() takes and returns one part's arrays. A program takes and returns all parts, laid end to end along the dimension named above; an argument that names none is the same for every part. Nothing has to cross between parts.
All inputs are finite; a program needn't handle non-finite values.
Results may differ from the reference program's by a relative error of at most 0.012.
Values may be sent and summed in bfloat16 or wider, within the bound.
A program may use at most 64 MiB of HBM per device.

```python
import math
import jax
import jax.numpy as jnp
from jax import lax

D = 2048
FF = 8192
FF_DEV = 2048
TOKENS = 2048
N_TP = 4


def draw_tokens(key, part):
    first = jax.random.fold_in(key, 11)
    second = jax.random.fold_in(key, 12)
    scales = jnp.exp(jax.random.uniform(second, (TOKENS, 1), jnp.float32, math.log(0.35), math.log(2.8)))
    base = jax.random.normal(first, (TOKENS, D), jnp.float32)
    return jnp.clip(base * scales, -12.0, 12.0).astype(jnp.bfloat16)


def block_scale(stream_key, extent, cuts, low, top_value):
    gain, own = 1.0, jax.random.fold_in(stream_key, 6)
    for position, shards_of in cuts:
        steps = jnp.exp(jax.random.uniform(jax.random.fold_in(own, position), (shards_of,), jnp.float32, low / len(cuts), top_value / len(cuts)))
        gain = gain * jnp.repeat(steps, extent[position] // shards_of).reshape([-1 if axis == position else 1 for axis in range(len(extent))])
    return gain


def gaussian(rng, dims, spread, bound, cuts=(), dtype=jnp.bfloat16):
    entries = jax.random.normal(rng, dims, jnp.float32) * spread
    if len(cuts) > 0:
        entries = block_scale(rng, dims, cuts, -0.22, 0.18) * entries
    return jnp.clip(entries, min=-bound, max=bound).astype(dtype)


def setup_inputs(seed: int = 0, part: int = 0) -> dict:
    key_list = jax.random.split(jax.random.key(seed), 5)
    own_keys = jax.random.split(jax.random.fold_in(key_list[4], part), 5)
    tokens = draw_tokens(jax.random.fold_in(jax.random.fold_in(key_list[4], part), 71), part)
    norm_gain = jnp.clip(1.0 + 0.18 * jax.random.normal(key_list[1], (D,), jnp.float32), 0.1, 1.9)
    w_in = gaussian(key_list[2], (D, FF), D ** -0.5, 0.125, ((0, 4), (1, 4)))
    w_out = gaussian(key_list[3], (FF, D), FF ** -0.5, 0.0625, ((0, 4), (1, 4)))
    return dict(tokens=tokens, norm_gain=norm_gain, w_in=w_in, w_out=w_out)


EPS = 1e-06

def reference(tokens, norm_gain, w_in, w_out):
    block = math.gcd(TOKENS, 2048)
    pieces = tokens.reshape(TOKENS // block, block, D)

    def one_block(rows_in):
        xf = rows_in.astype(jnp.float32)
        scale = lax.rsqrt(lax.optimization_barrier(jnp.mean(xf * xf, axis=-1, keepdims=True)) + EPS)
        normed = (xf * scale * norm_gain.astype(jnp.float32)).astype(jnp.bfloat16)
        pre = jnp.dot(normed, w_in, preferred_element_type=jnp.float32)
        hidden = jnp.square(jax.nn.relu(pre)).astype(jnp.bfloat16)
        total = xf
        for index in range(N_TP):
            lower = index * FF_DEV
            partial_sum = jnp.dot(hidden[:, lower:lower + FF_DEV], w_out[lower:lower + FF_DEV, :], preferred_element_type=jnp.float32).astype(jnp.bfloat16)
            partial_sum = lax.optimization_barrier(partial_sum)
            total = total + partial_sum.astype(jnp.float32)
        return total.astype(jnp.bfloat16)
    mixed = lax.map(one_block, pieces)
    return mixed.reshape(TOKENS, D)
```

```python
import functools

import jax
import jax.numpy as jnp
from jax import lax
from jax.experimental import pallas as pl
from jax.experimental.pallas import tpu as pltpu
from jax.sharding import PartitionSpec as P

EPS = 1e-06
MESH = pl.DeviceIdType.MESH
CORES = 2
PLANES = 2
LAG_1, LAG_2, LAG_3, LAG_4 = 1, 3, 6, 8


def remote(src, dst, send, recv, device):
    pltpu.make_async_remote_copy(
        src_ref=src, dst_ref=dst, send_sem=send, recv_sem=recv, device_id=device, device_id_type=MESH
    ).start()


def done(ref, sem):
    pltpu.make_async_copy(ref, ref, sem).wait()


def f32(value):
    return value.astype(jnp.float32)


def kernel(
    Y, n, X, parts, x_hbm, g_ref, wi_ref, wo_ref, o_hbm,
    norm, wi, wo, hid, crecv, yl, xf, xl, yf, own_l, own_f, zsend, zrecv, x_ref, out,
    x_sem, o_sem, tok_send, tok_recv, wi_send, wi_recv, wo_send, wo_recv, wi_fwd, wo_fwd,
    c_send, c_recv, yl_send, yl_recv, xf_send, xf_recv, xl_send, xl_recv, yf_send, yf_recv, z_send, z_recv,
):
    y, i, j = lax.axis_index("grp"), lax.axis_index("fs"), lax.axis_index("tp")
    x, core, zp = j // CORES, j % CORES, i % PLANES
    chips = Y * X
    B, D = x_ref.shape
    HU = wi.shape[1]
    Dr, Dc = wi_ref.shape[0], wo_ref.shape[1]
    W = Dc // parts
    NC = n * parts
    R = norm.shape[0]
    half = R // CORES
    region = chips * B

    partner = (y, i, x * CORES + 1 - core)
    near = i + 1 - 2 * zp
    zpair = (y, near, j)

    def plane(d):
        return (y, d, j)

    def at(yy, xx):
        return (yy, i, xx * CORES + core)

    def turn(v, o, size):
        return lax.rem(v + o, size)

    others = [(oy, ox) for oy in range(Y) for ox in range(X) if oy or ox]

    def has(d):
        return (d >= 0) & (d < n)

    HOPS = (1, 2, -1, -2)

    load_x = pltpu.make_async_copy(x_hbm, x_ref, x_sem)
    load_x.start()

    barrier = pltpu.get_barrier_semaphore()
    peers = len(others) + 1
    for step in HOPS:
        there = has(i + step)
        peers += there.astype(jnp.int32)

        @pl.when(there)
        def _():
            pl.semaphore_signal(barrier, inc=1, device_id=plane(i + step), device_id_type=MESH)

    pl.semaphore_signal(barrier, inc=1, device_id=partner, device_id_type=MESH)
    for oy, ox in others:
        pl.semaphore_signal(
            barrier, inc=1, device_id=at(turn(y, oy, Y), turn(x, ox, X)), device_id_type=MESH
        )

    def block_l(c, yy, xx):
        return c * PLANES * chips + yy * X + xx

    def block_f(c, yy, xx):
        return (c * PLANES + 1) * chips + xx * Y + yy

    def rows_at(first, size):
        return pl.ds(pl.multiple_of(first, B), size)

    def rows_of(b):
        return rows_at(b * B, B)

    mine, paired = block_l(core, y, x), block_f(core, y, x)

    def in_cols(d):
        return pl.ds(pl.multiple_of(((d % PLANES) * Y + y) * HU, HU), HU)

    def in_rows(s):
        return pl.ds(pl.multiple_of(s * Dr, Dr), Dr)

    def out_cols(cid):
        return pl.ds(pl.multiple_of(cid * W, W), W)

    pltpu.make_async_copy(wi_ref.at[:, in_cols(i)], wi.at[in_rows(i), :], wi_recv.at[i]).start()
    for h in range(parts):
        cid = i * parts + h
        pltpu.make_async_copy(
            wo_ref.at[in_cols(i), pl.ds(h * W, W)], wo.at[:, out_cols(cid)], wo_recv.at[cid]
        ).start()

    load_x.wait()

    @pl.loop(0, B // 16)
    def _(r):
        rows = pl.ds(pl.multiple_of(r * 16, 16), 16)
        v = f32(x_ref[rows, :])
        scale = lax.rsqrt(jnp.mean(v * v, axis=-1, keepdims=True) + EPS)
        out_rows = pl.ds(pl.multiple_of(mine * B + r * 16, 16), 16)
        norm[out_rows, :] = (v * scale * g_ref[...]).astype(jnp.bfloat16)

    pl.semaphore_wait(barrier, peers)

    def send_in(step):
        d = i + step
        k = HOPS.index(step)

        @pl.when(has(d))
        def _():
            remote(wi_ref.at[:, in_cols(d)], wi.at[in_rows(i), :], wi_send.at[k], wi_recv.at[i], plane(d))

    def send_out(h, step):
        d = i + step
        k = HOPS.index(step)

        @pl.when(has(d))
        def _():
            cid = i * parts + h
            remote(
                wo_ref.at[in_cols(d), pl.ds(pl.multiple_of(h * W, W), W)], wo.at[:, out_cols(cid)],
                wo_send.at[h, k], wo_recv.at[cid], plane(d),
            )

    def both_ways(send):
        for sign in (1, -1):
            relayed = has(i + 3 * sign)

            @pl.when(relayed)
            def _():
                send(sign)
                send(2 * sign)

            @pl.when(jnp.logical_not(relayed))
            def _():
                send(2 * sign)
                send(sign)

    def onward(s):
        return jnp.where(s < i, i + 2, i - 2)

    def relays(s):
        return (s != i) & has(onward(s))

    def relay_in(s):
        @pl.when(relays(s))
        def _():
            ref = wi.at[in_rows(s), :]
            remote(ref, ref, wi_fwd.at[s], wi_recv.at[s], plane(onward(s)))

    def relay_out(cid):
        s = cid // parts

        @pl.when(relays(s))
        def _():
            ref = wo.at[:, out_cols(cid)]
            remote(ref, ref, wo_fwd.at[cid], wo_recv.at[cid], plane(onward(s)))

    count = [0]

    def send_block(b, device, into=None):
        into = b if into is None else into
        remote(
            norm.at[rows_of(b), :], norm.at[rows_of(into), :],
            tok_send.at[count[0]], tok_recv.at[into], device,
        )
        count[0] += 1

    send_block(mine, zpair, paired)
    both_ways(send_in)
    for oy, ox in others:
        send_block(mine, at(turn(y, oy, Y), turn(x, ox, X)))
    send_block(mine, partner)

    def arrived(b):
        done(norm.at[rows_of(b), :], tok_recv.at[b])

    arrived(paired)
    for oy, ox in others:
        send_block(paired, at(turn(y, oy, Y), turn(x, ox, X)))
    send_block(paired, partner)

    def in_arrived(s):
        done(wi.at[in_rows(s), :], wi_recv.at[s])
        relay_in(s)

    def source(k):
        if k == 0:
            return i
        if k == 1:
            return near
        pair = lax.rem(i // PLANES + k // PLANES, n // PLANES)
        e = k % PLANES
        return jnp.where(pair > i // PLANES, pair * PLANES + e, pair * PLANES + PLANES - 1 - e)

    inner = relays(near)

    @pl.when(jnp.logical_not(inner))
    def _():
        for h in range(parts):
            both_ways(functools.partial(send_out, h))

    in_arrived(source(1))

    @pl.when(inner)
    def _():
        both_ways(functools.partial(send_out, 0))

    def near_out(h):
        cid = near * parts + h
        done(wo.at[:, out_cols(cid)], wo_recv.at[cid])

        @pl.when(inner)
        def _():
            relay_out(cid)
            pl.when(h + 1 < parts)(lambda: both_ways(functools.partial(send_out, h + 1)))

    for block in (block_l, block_f):
        for oy, ox in others:
            b = block(core, turn(y, Y - oy, Y), turn(x, X - ox, X))
            arrived(b)
            send_block(b, partner)
    for yy in range(Y):
        for xx in range(X):
            arrived(block_l(1 - core, yy, xx))
            arrived(block_f(1 - core, yy, xx))

    in_arrived(source(0))
    for k in range(2, n):
        in_arrived(source(k))

    near_out(0)

    TR = min(512, half)

    @pl.loop(0, R // TR)
    def _(r):
        rows = pl.ds(pl.multiple_of(r * TR, TR), TR)
        pre = jnp.dot(norm[rows, :], wi[...], preferred_element_type=jnp.float32)
        hid[rows, :] = jnp.square(jnp.maximum(pre, 0.0)).astype(jnp.bfloat16)

    for q in range(count[0]):
        done(norm.at[rows_of(0), :], tok_send.at[q])

    kept, given = core * half, (1 - core) * half

    def chunk(t):
        k, h = t % n, t // n
        pair = lax.rem(i // PLANES + k // PLANES, n // PLANES)
        e = k % PLANES
        far = jnp.where(pair > i // PLANES, pair * PLANES + e, pair * PLANES + PLANES - 1 - e)
        s = jnp.where(k == 0, near, jnp.where(k == 1, i, far))
        return s * parts + h

    TM = min(1024, half)

    def multiply(first, cols):
        for r in range(half // TM):
            rows = pl.ds(pl.multiple_of(first + r * TM, TM), TM)
            norm[rows, cols] = jnp.dot(
                hid[rows, :], wo[:, cols], preferred_element_type=jnp.float32
            ).astype(jnp.bfloat16)

    def fold(first, size, cols):
        rows = rows_at(kept + first, size)
        norm[rows, cols] = (f32(norm[rows, cols]) + f32(crecv[rows_at(first, size), cols])).astype(jnp.bfloat16)

    SL, SF = X * B, Y * B

    def part_sum(first, cols, landed, others_of, inside):
        v = f32(norm[rows_at(kept + first, B), cols]) + f32(crecv[rows_at(first, B), cols])
        for o in others_of:
            v += f32(landed[o, rows_at(inside, B), cols])
        return v

    def product(t):
        cid = chunk(t)
        cols = out_cols(cid)
        k, h = t % n, t // n

        @pl.when(k > 0)
        def _():
            done(wo.at[:, cols], wo_recv.at[cid])
            relay_out(cid)

        pl.when((k == 1) & (h + 1 < parts))(lambda: near_out(h + 1))

        multiply(given, cols)
        remote(
            norm.at[rows_at(given, half), cols], crecv.at[:, cols], c_send, c_recv.at[cid], partner
        )
        multiply(kept, cols)

    def first_stage(t):
        cid = chunk(t)
        cols = out_cols(cid)
        done(crecv.at[:, cols], c_recv.at[cid])
        for o in range(1, X):
            xx = turn(x, o, X)
            fold(region + xx * SF, SF, cols)
            remote(
                norm.at[rows_at(kept + region + xx * SF, SF), cols], xf.at[x, :, cols],
                xf_send, xf_recv.at[cid * X + x], at(y, xx),
            )
        for o in range(1, Y):
            yy = turn(y, o, Y)
            fold(yy * SL, SL, cols)
            remote(
                norm.at[rows_at(kept + yy * SL, SL), cols], yl.at[y, :, cols],
                yl_send, yl_recv.at[cid * Y + y], at(yy, x),
            )

    def second_stage(t):
        cid = chunk(t)
        cols = out_cols(cid)
        xs = [turn(x, o, X) for o in range(1, X)]
        ys = [turn(y, o, Y) for o in range(1, Y)]
        for xx in xs:
            done(xf.at[xx, :, cols], xf_recv.at[cid * X + xx])
        for yy in ys:
            first = region + x * SF + yy * B
            norm[rows_at(kept + first, B), cols] = part_sum(first, cols, xf, xs, yy * B).astype(jnp.bfloat16)
            remote(
                norm.at[rows_at(kept + first, B), cols], yf.at[y, :, cols],
                yf_send, yf_recv.at[cid * Y + y], at(yy, x),
            )
        for yy in ys:
            done(yl.at[yy, :, cols], yl_recv.at[cid * Y + yy])
        for xx in xs:
            first = y * SL + xx * B
            norm[rows_at(kept + first, B), cols] = part_sum(first, cols, yl, ys, xx * B).astype(jnp.bfloat16)
            remote(
                norm.at[rows_at(kept + first, B), cols], xl.at[x, :, cols],
                xl_send, xl_recv.at[cid * X + x], at(y, xx),
            )
        own_f[:, cols] = part_sum(region + x * SF + y * B, cols, xf, xs, y * B)
        own_l[:, cols] = part_sum(y * SL + x * B, cols, yl, ys, x * B)

    def third_stage(t):
        cid = chunk(t)
        cols = out_cols(cid)
        v = own_f[:, cols]
        for o in range(1, Y):
            yy = turn(y, o, Y)
            done(yf.at[yy, :, cols], yf_recv.at[cid * Y + yy])
            v += f32(yf[yy, :, cols])
        zsend[:, cols] = v.astype(jnp.bfloat16)
        remote(zsend.at[:, cols], zrecv.at[:, cols], z_send, z_recv.at[cid], zpair)
        v = own_l[:, cols]
        for o in range(1, X):
            xx = turn(x, o, X)
            done(xl.at[xx, :, cols], xl_recv.at[cid * X + xx])
            v += f32(xl[xx, :, cols])
        own_l[:, cols] = v

    def finish(t):
        cid = chunk(t)
        cols = out_cols(cid)
        done(zrecv.at[:, cols], z_recv.at[cid])
        v = own_l[:, cols] + f32(zrecv[:, cols])
        out[:, cols] = (f32(x_ref[:, cols]) + v).astype(jnp.bfloat16)
        pltpu.make_async_copy(out.at[:, cols], o_hbm.at[:, cols], o_sem).start()

    stages = ((0, product), (LAG_1, first_stage), (LAG_2, second_stage), (LAG_3, third_stage), (LAG_4, finish))

    @pl.loop(0, NC + LAG_4)
    def _(t):
        for lag, stage in stages:
            pl.when((t >= lag) & (t < NC + lag))(functools.partial(stage, t - lag))

    for k, step in enumerate(HOPS):
        @pl.when(has(i + step))
        def _():
            done(wi.at[in_rows(0), :], wi_send.at[k])
            for h in range(parts):
                done(wo.at[:, out_cols(0)], wo_send.at[h, k])

    for s in range(n):
        @pl.when(relays(s))
        def _():
            done(wi.at[in_rows(0), :], wi_fwd.at[s])
            for h in range(parts):
                done(wo.at[:, out_cols(0)], wo_fwd.at[s * parts + h])

    done(crecv, c_send)
    if Y > 1:
        done(yl.at[pl.ds(0, Y - 1)], yl_send)
        done(yf.at[pl.ds(0, Y - 1)], yf_send)
    if X > 1:
        done(xf.at[pl.ds(0, X - 1)], xf_send)
        done(xl.at[pl.ds(0, X - 1)], xl_send)
    done(zsend, z_send)
    pltpu.make_async_copy(out, o_hbm, o_sem).wait()


def solution(mesh):
    Y, n, T = mesh.shape["grp"], mesh.shape["fs"], mesh.shape["tp"]
    X = T // CORES
    chips = Y * X

    def local(tokens, norm_gain, w_in, w_out):
        B, D = tokens.shape
        HU = w_in.shape[1] // (PLANES * Y)
        parts = w_out.shape[1] // 128
        NC = n * parts
        R = CORES * chips * PLANES * B
        sends = 1 + 2 * chips + PLANES * (chips - 1)
        bf16 = jnp.bfloat16
        dma = pltpu.SemaphoreType.DMA
        vmem = pl.BlockSpec(memory_space=pltpu.VMEM)
        hbm = pl.BlockSpec(memory_space=pl.ANY)
        return pl.pallas_call(
            functools.partial(kernel, Y, n, X, parts),
            out_shape=jax.ShapeDtypeStruct((B, D), bf16),
            in_specs=[hbm, vmem, hbm, hbm],
            out_specs=hbm,
            scratch_shapes=[
                pltpu.VMEM((R, D), bf16),
                pltpu.VMEM((D, HU), bf16),
                pltpu.VMEM((HU, D), bf16),
                pltpu.VMEM((R, HU), bf16),
                pltpu.VMEM((R // CORES, D), bf16),
                pltpu.VMEM((Y, X * B, D), bf16),
                pltpu.VMEM((X, Y * B, D), bf16),
                pltpu.VMEM((X, B, D), bf16),
                pltpu.VMEM((Y, B, D), bf16),
                pltpu.VMEM((B, D), jnp.float32),
                pltpu.VMEM((B, D), jnp.float32),
                pltpu.VMEM((B, D), bf16),
                pltpu.VMEM((B, D), bf16),
                pltpu.VMEM((B, D), bf16),
                pltpu.VMEM((B, D), bf16),
                dma, dma,
                dma((sends,)), dma((CORES * chips * PLANES,)),
                dma((4,)), dma((n,)),
                dma((parts, 4)), dma((NC,)),
                dma((n,)), dma((NC,)),
                dma, dma((NC,)),
                dma, dma((NC * Y,)),
                dma, dma((NC * X,)),
                dma, dma((NC * X,)),
                dma, dma((NC * Y,)),
                dma, dma((NC,)),
            ],
            compiler_params=pltpu.CompilerParams(
                collective_id=0, has_side_effects=True, vmem_limit_bytes=60 * 1024 * 1024
            ),
        )(tokens, norm_gain.reshape(1, D), w_in, w_out)

    in_specs = (P(("grp", "fs", "tp"), None), P(), P("fs", "tp"), P("tp", "fs"))
    out_specs = P(("grp", "fs", "tp"), None)
    return jax.shard_map(local, mesh=mesh, in_specs=in_specs, out_specs=out_specs, check_vma=False)
```

```python
import functools

import jax
import jax.numpy as jnp
from jax import lax
from jax.experimental import pallas as pl
from jax.experimental.pallas import tpu as pltpu
from jax.sharding import PartitionSpec as P

EPS = 1e-06
MESH = pl.DeviceIdType.MESH
CORES = 2
PLANES = 2
FAR_STEP = 0.0
LAG_1, LAG_2, LAG_3, LAG_4 = 1, 3, 5, 7


def remote(src, dst, send, recv, device):
    pltpu.make_async_remote_copy(
        src_ref=src, dst_ref=dst, send_sem=send, recv_sem=recv, device_id=device, device_id_type=MESH
    ).start()


def done(ref, sem):
    pltpu.make_async_copy(ref, ref, sem).wait()


def f32(value):
    return value.astype(jnp.float32)


def kernel(
    Y, n, X, parts, x_hbm, g_ref, wi_ref, wo_ref, o_hbm,
    norm, wi, wo, hid, crecv, yl, xf, xl, yf, own_l, own_f, zsend, zrecv, x_ref, out,
    x_sem, o_sem, tok_send, tok_recv, wi_send, wi_recv, wo_send, wo_recv, wi_fwd, wo_fwd,
    c_send, c_recv, yl_send, yl_recv, xf_send, xf_recv, xl_send, xl_recv, yf_send, yf_recv, z_send, z_recv,
):
    y, i, j = lax.axis_index("grp"), lax.axis_index("fs"), lax.axis_index("tp")
    x, core, zp = j // CORES, j % CORES, i % PLANES
    chips = Y * X
    B, D = x_ref.shape
    HU = wi.shape[1]
    Dr, Dc = wi_ref.shape[0], wo_ref.shape[1]
    W = Dc // parts
    NC = n * parts
    R = norm.shape[0]
    half = R // CORES
    region = chips * B

    partner = (y, i, x * CORES + 1 - core)
    near = i + 1 - 2 * zp
    zpair = (y, near, j)

    def plane(d):
        return (y, d, j)

    def at(yy, xx):
        return (yy, i, xx * CORES + core)

    def turn(v, o, size):
        return lax.rem(v + o, size)

    others = [(oy, ox) for oy in range(Y) for ox in range(X) if oy or ox]

    def has(d):
        return (d >= 0) & (d < n)

    HOPS = (1, 2, -1, -2)

    load_x = pltpu.make_async_copy(x_hbm, x_ref, x_sem)
    load_x.start()

    barrier = pltpu.get_barrier_semaphore()
    peers = len(others) + 1
    for step in HOPS:
        there = has(i + step)
        peers += there.astype(jnp.int32)

        @pl.when(there)
        def _():
            pl.semaphore_signal(barrier, inc=1, device_id=plane(i + step), device_id_type=MESH)

    pl.semaphore_signal(barrier, inc=1, device_id=partner, device_id_type=MESH)
    for oy, ox in others:
        pl.semaphore_signal(
            barrier, inc=1, device_id=at(turn(y, oy, Y), turn(x, ox, X)), device_id_type=MESH
        )

    def block_l(c, yy, xx):
        return c * PLANES * chips + yy * X + xx

    def block_f(c, yy, xx):
        return (c * PLANES + 1) * chips + xx * Y + yy

    def rows_at(first, size):
        return pl.ds(pl.multiple_of(first, B), size)

    def rows_of(b):
        return rows_at(b * B, B)

    mine, paired = block_l(core, y, x), block_f(core, y, x)

    def in_cols(d):
        return pl.ds(pl.multiple_of(((d % PLANES) * Y + y) * HU, HU), HU)

    def in_rows(s):
        return pl.ds(pl.multiple_of(s * Dr, Dr), Dr)

    def out_cols(cid):
        return pl.ds(pl.multiple_of(cid * W, W), W)

    pltpu.make_async_copy(wi_ref.at[:, in_cols(i)], wi.at[in_rows(i), :], wi_recv.at[i]).start()
    for h in range(parts):
        cid = i * parts + h
        pltpu.make_async_copy(
            wo_ref.at[in_cols(i), pl.ds(h * W, W)], wo.at[:, out_cols(cid)], wo_recv.at[cid]
        ).start()

    load_x.wait()

    @pl.loop(0, B // 16)
    def _(r):
        rows = pl.ds(pl.multiple_of(r * 16, 16), 16)
        v = f32(x_ref[rows, :])
        scale = lax.rsqrt(jnp.mean(v * v, axis=-1, keepdims=True) + EPS)
        out_rows = pl.ds(pl.multiple_of(mine * B + r * 16, 16), 16)
        norm[out_rows, :] = (v * scale * g_ref[...]).astype(jnp.bfloat16)

    pl.semaphore_wait(barrier, peers)

    def send_in(step):
        d = i + step
        k = HOPS.index(step)

        @pl.when(has(d))
        def _():
            remote(wi_ref.at[:, in_cols(d)], wi.at[in_rows(i), :], wi_send.at[k], wi_recv.at[i], plane(d))

    def send_out(h, step):
        d = i + step
        k = HOPS.index(step)

        @pl.when(has(d))
        def _():
            cid = i * parts + h
            remote(
                wo_ref.at[in_cols(d), pl.ds(pl.multiple_of(h * W, W), W)], wo.at[:, out_cols(cid)],
                wo_send.at[h, k], wo_recv.at[cid], plane(d),
            )

    def both_ways(send):
        for sign in (1, -1):
            relayed = has(i + 3 * sign)

            @pl.when(relayed)
            def _():
                send(sign)
                send(2 * sign)

            @pl.when(jnp.logical_not(relayed))
            def _():
                send(2 * sign)
                send(sign)

    def onward(s):
        return jnp.where(s < i, i + 2, i - 2)

    def relays(s):
        return (s != i) & has(onward(s))

    def relay_in(s):
        @pl.when(relays(s))
        def _():
            ref = wi.at[in_rows(s), :]
            remote(ref, ref, wi_fwd.at[s], wi_recv.at[s], plane(onward(s)))

    def relay_out(cid):
        s = cid // parts

        @pl.when(relays(s))
        def _():
            ref = wo.at[:, out_cols(cid)]
            remote(ref, ref, wo_fwd.at[cid], wo_recv.at[cid], plane(onward(s)))

    count = [0]

    def send_block(b, device, into=None):
        into = b if into is None else into
        remote(
            norm.at[rows_of(b), :], norm.at[rows_of(into), :],
            tok_send.at[count[0]], tok_recv.at[into], device,
        )
        count[0] += 1

    send_block(mine, zpair, paired)
    both_ways(send_in)
    for oy, ox in others:
        send_block(mine, at(turn(y, oy, Y), turn(x, ox, X)))
    send_block(mine, partner)

    def arrived(b):
        done(norm.at[rows_of(b), :], tok_recv.at[b])

    arrived(paired)
    for oy, ox in others:
        send_block(paired, at(turn(y, oy, Y), turn(x, ox, X)))
    send_block(paired, partner)

    def in_arrived(s):
        done(wi.at[in_rows(s), :], wi_recv.at[s])
        relay_in(s)

    def source(k):
        if k == 0:
            return i
        if k == 1:
            return near
        pair = lax.rem(i // PLANES + k // PLANES, n // PLANES)
        e = k % PLANES
        return jnp.where(pair > i // PLANES, pair * PLANES + e, pair * PLANES + PLANES - 1 - e)

    inner = relays(near)

    def out_near(h):
        for step in (1, -1):
            pl.when(i + step == near)(functools.partial(send_out, h, step))

    def out_far(h):
        for step in (2, 1, -2, -1):
            pl.when(i + step != near)(functools.partial(send_out, h, step))

    def outer_out():
        for h in range(parts):
            out_near(h)
        for h in range(parts):
            out_far(h)

    pl.when(jnp.logical_not(inner))(outer_out)
    in_arrived(source(1))

    @pl.when(inner)
    def _():
        for h in range(parts):
            out_near(h)
        out_far(0)

    def near_out(h):
        cid = near * parts + h
        done(wo.at[:, out_cols(cid)], wo_recv.at[cid])

        @pl.when(inner)
        def _():
            relay_out(cid)
            pl.when(h + 1 < parts)(lambda: out_far(h + 1))

    for block in (block_l, block_f):
        for oy, ox in others:
            b = block(core, turn(y, Y - oy, Y), turn(x, X - ox, X))
            arrived(b)
            send_block(b, partner)
    for yy in range(Y):
        for xx in range(X):
            arrived(block_l(1 - core, yy, xx))
            arrived(block_f(1 - core, yy, xx))

    in_arrived(source(0))
    for k in range(2, n):
        in_arrived(source(k))

    near_out(0)

    TR = min(512, half)

    @pl.loop(0, R // TR)
    def _(r):
        rows = pl.ds(pl.multiple_of(r * TR, TR), TR)
        pre = jnp.dot(norm[rows, :], wi[...], preferred_element_type=jnp.float32)
        hid[rows, :] = jnp.square(jnp.maximum(pre, 0.0)).astype(jnp.bfloat16)

    for q in range(count[0]):
        done(norm.at[rows_of(0), :], tok_send.at[q])

    kept, given = core * half, (1 - core) * half

    ready = [(k, h) for k in (1, 0) for h in range(parts)]
    later = [(k, h) for k in range(2, n) for h in range(parts)]
    later.sort(key=lambda v: (v[1] + FAR_STEP * (v[0] - 2), v[0]))

    def chunk(t):
        code = jnp.int32(0)
        for q, (k, h) in enumerate(ready + later):
            code = jnp.where(t == q, k * parts + h, code)
        k, h = code // parts, code % parts
        pair = lax.rem(i // PLANES + k // PLANES, n // PLANES)
        e = k % PLANES
        far = jnp.where(pair > i // PLANES, pair * PLANES + e, pair * PLANES + PLANES - 1 - e)
        s = jnp.where(k == 0, near, jnp.where(k == 1, i, far))
        return s * parts + h

    TM = min(1024, half)

    def multiply(first, cols):
        for r in range(half // TM):
            rows = pl.ds(pl.multiple_of(first + r * TM, TM), TM)
            norm[rows, cols] = jnp.dot(
                hid[rows, :], wo[:, cols], preferred_element_type=jnp.float32
            ).astype(jnp.bfloat16)

    def fold(first, size, cols):
        rows = rows_at(kept + first, size)
        norm[rows, cols] = (f32(norm[rows, cols]) + f32(crecv[rows_at(first, size), cols])).astype(jnp.bfloat16)

    SL, SF = X * B, Y * B

    def part_sum(first, cols, landed, others_of, inside):
        v = f32(norm[rows_at(kept + first, B), cols]) + f32(crecv[rows_at(first, B), cols])
        for o in others_of:
            v += f32(landed[o, rows_at(inside, B), cols])
        return v

    def product(t):
        cid = chunk(t)
        cols = out_cols(cid)

        @pl.when(cid // parts != near)
        def _():
            done(wo.at[:, cols], wo_recv.at[cid])
            relay_out(cid)

        pl.when(t + 1 < parts)(lambda: near_out(t + 1))

        multiply(given, cols)
        remote(
            norm.at[rows_at(given, half), cols], crecv.at[:, cols], c_send, c_recv.at[cid], partner
        )
        multiply(kept, cols)

    def first_stage(t):
        cid = chunk(t)
        cols = out_cols(cid)
        done(crecv.at[:, cols], c_recv.at[cid])
        for o in range(1, X):
            xx = turn(x, o, X)
            fold(region + xx * SF, SF, cols)
            remote(
                norm.at[rows_at(kept + region + xx * SF, SF), cols], xf.at[x, :, cols],
                xf_send, xf_recv.at[cid * X + x], at(y, xx),
            )
        for o in range(1, Y):
            yy = turn(y, o, Y)
            fold(yy * SL, SL, cols)
            remote(
                norm.at[rows_at(kept + yy * SL, SL), cols], yl.at[y, :, cols],
                yl_send, yl_recv.at[cid * Y + y], at(yy, x),
            )

    def second_stage(t):
        cid = chunk(t)
        cols = out_cols(cid)
        xs = [turn(x, o, X) for o in range(1, X)]
        ys = [turn(y, o, Y) for o in range(1, Y)]
        for xx in xs:
            done(xf.at[xx, :, cols], xf_recv.at[cid * X + xx])
        for yy in ys:
            first = region + x * SF + yy * B
            norm[rows_at(kept + first, B), cols] = part_sum(first, cols, xf, xs, yy * B).astype(jnp.bfloat16)
            remote(
                norm.at[rows_at(kept + first, B), cols], yf.at[y, :, cols],
                yf_send, yf_recv.at[cid * Y + y], at(yy, x),
            )
        for yy in ys:
            done(yl.at[yy, :, cols], yl_recv.at[cid * Y + yy])
        for xx in xs:
            first = y * SL + xx * B
            norm[rows_at(kept + first, B), cols] = part_sum(first, cols, yl, ys, xx * B).astype(jnp.bfloat16)
            remote(
                norm.at[rows_at(kept + first, B), cols], xl.at[x, :, cols],
                xl_send, xl_recv.at[cid * X + x], at(y, xx),
            )
        own_f[:, cols] = part_sum(region + x * SF + y * B, cols, xf, xs, y * B)
        own_l[:, cols] = part_sum(y * SL + x * B, cols, yl, ys, x * B)

    def third_stage(t):
        cid = chunk(t)
        cols = out_cols(cid)
        v = own_f[:, cols]
        for o in range(1, Y):
            yy = turn(y, o, Y)
            done(yf.at[yy, :, cols], yf_recv.at[cid * Y + yy])
            v += f32(yf[yy, :, cols])
        zsend[:, cols] = v.astype(jnp.bfloat16)
        remote(zsend.at[:, cols], zrecv.at[:, cols], z_send, z_recv.at[cid], zpair)
        v = own_l[:, cols]
        for o in range(1, X):
            xx = turn(x, o, X)
            done(xl.at[xx, :, cols], xl_recv.at[cid * X + xx])
            v += f32(xl[xx, :, cols])
        own_l[:, cols] = v

    def finish(t):
        cid = chunk(t)
        cols = out_cols(cid)
        done(zrecv.at[:, cols], z_recv.at[cid])
        v = own_l[:, cols] + f32(zrecv[:, cols])
        out[:, cols] = (f32(x_ref[:, cols]) + v).astype(jnp.bfloat16)
        pltpu.make_async_copy(out.at[:, cols], o_hbm.at[:, cols], o_sem).start()

    def finish_far(t):
        pl.when(t >= len(ready))(lambda: finish(t))

    def finish_ready(t):
        pl.when(t < len(ready))(lambda: finish(t))

    LAG_5 = LAG_4 + parts
    stages = ((0, product), (LAG_1, first_stage), (LAG_2, second_stage), (LAG_3, third_stage),
              (LAG_4, finish_far), (LAG_5, finish_ready))

    @pl.loop(0, NC + LAG_4)
    def _(t):
        for lag, stage in stages:
            pl.when((t >= lag) & (t < NC + lag))(functools.partial(stage, t - lag))

    for k, step in enumerate(HOPS):
        @pl.when(has(i + step))
        def _():
            done(wi.at[in_rows(0), :], wi_send.at[k])
            for h in range(parts):
                done(wo.at[:, out_cols(0)], wo_send.at[h, k])

    for s in range(n):
        @pl.when(relays(s))
        def _():
            done(wi.at[in_rows(0), :], wi_fwd.at[s])
            for h in range(parts):
                done(wo.at[:, out_cols(0)], wo_fwd.at[s * parts + h])

    done(crecv, c_send)
    if Y > 1:
        done(yl.at[pl.ds(0, Y - 1)], yl_send)
        done(yf.at[pl.ds(0, Y - 1)], yf_send)
    if X > 1:
        done(xf.at[pl.ds(0, X - 1)], xf_send)
        done(xl.at[pl.ds(0, X - 1)], xl_send)
    done(zsend, z_send)
    pltpu.make_async_copy(out, o_hbm, o_sem).wait()


def solution(mesh):
    Y, n, T = mesh.shape["grp"], mesh.shape["fs"], mesh.shape["tp"]
    X = T // CORES
    chips = Y * X

    def local(tokens, norm_gain, w_in, w_out):
        B, D = tokens.shape
        HU = w_in.shape[1] // (PLANES * Y)
        parts = w_out.shape[1] // 128
        NC = n * parts
        R = CORES * chips * PLANES * B
        sends = 1 + 2 * chips + PLANES * (chips - 1)
        bf16 = jnp.bfloat16
        dma = pltpu.SemaphoreType.DMA
        vmem = pl.BlockSpec(memory_space=pltpu.VMEM)
        hbm = pl.BlockSpec(memory_space=pl.ANY)
        return pl.pallas_call(
            functools.partial(kernel, Y, n, X, parts),
            out_shape=jax.ShapeDtypeStruct((B, D), bf16),
            in_specs=[hbm, vmem, hbm, hbm],
            out_specs=hbm,
            scratch_shapes=[
                pltpu.VMEM((R, D), bf16),
                pltpu.VMEM((D, HU), bf16),
                pltpu.VMEM((HU, D), bf16),
                pltpu.VMEM((R, HU), bf16),
                pltpu.VMEM((R // CORES, D), bf16),
                pltpu.VMEM((Y, X * B, D), bf16),
                pltpu.VMEM((X, Y * B, D), bf16),
                pltpu.VMEM((X, B, D), bf16),
                pltpu.VMEM((Y, B, D), bf16),
                pltpu.VMEM((B, D), jnp.float32),
                pltpu.VMEM((B, D), jnp.float32),
                pltpu.VMEM((B, D), bf16),
                pltpu.VMEM((B, D), bf16),
                pltpu.VMEM((B, D), bf16),
                pltpu.VMEM((B, D), bf16),
                dma, dma,
                dma((sends,)), dma((CORES * chips * PLANES,)),
                dma((4,)), dma((n,)),
                dma((parts, 4)), dma((NC,)),
                dma((n,)), dma((NC,)),
                dma, dma((NC,)),
                dma, dma((NC * Y,)),
                dma, dma((NC * X,)),
                dma, dma((NC * X,)),
                dma, dma((NC * Y,)),
                dma, dma((NC,)),
            ],
            compiler_params=pltpu.CompilerParams(
                collective_id=0, has_side_effects=True, vmem_limit_bytes=60 * 1024 * 1024
            ),
        )(tokens, norm_gain.reshape(1, D), w_in, w_out)

    in_specs = (P(("grp", "fs", "tp"), None), P(), P("fs", "tp"), P("tp", "fs"))
    out_specs = P(("grp", "fs", "tp"), None)
    return jax.shard_map(local, mesh=mesh, in_specs=in_specs, out_specs=out_specs, check_vma=False)
```

```python
import functools

import jax
import jax.numpy as jnp
from jax import lax
from jax.experimental import pallas as pl
from jax.experimental.pallas import tpu as pltpu
from jax.sharding import PartitionSpec as P

EPS = 1e-06
MESH = pl.DeviceIdType.MESH
CORES = 2
PLANES = 2
FAR_STEP = 0.0
LAG_1, LAG_2, LAG_3, LAG_4 = 1, 3, 5, 7


def remote(src, dst, send, recv, device):
    pltpu.make_async_remote_copy(
        src_ref=src, dst_ref=dst, send_sem=send, recv_sem=recv, device_id=device, device_id_type=MESH
    ).start()


def done(ref, sem):
    pltpu.make_async_copy(ref, ref, sem).wait()


def f32(value):
    return value.astype(jnp.float32)


def kernel(
    Y, n, X, parts, x_hbm, g_hbm, wi_ref, wo_ref, o_hbm,
    norm, wi, wo, hid, crecv, yl, xf, xl, yf, own_l, own_f, zsend, zrecv, x_ref, g_ref, out,
    x_sem, g_sem, o_sem, tok_send, tok_recv, wi_send, wi_recv, wo_send, wo_recv, wi_fwd, wo_fwd,
    c_send, c_recv, yl_send, yl_recv, xf_send, xf_recv, xl_send, xl_recv, yf_send, yf_recv, z_send, z_recv,
):
    y, i, j = lax.axis_index("grp"), lax.axis_index("fs"), lax.axis_index("tp")
    x, core, zp = j // CORES, j % CORES, i % PLANES
    chips = Y * X
    B, D = x_ref.shape
    HU = wi.shape[1]
    Dr, Dc = wi_ref.shape[0], wo_ref.shape[1]
    W = Dc // parts
    NC = n * parts
    R = norm.shape[0]
    half = R // CORES
    region = chips * B

    partner = (y, i, x * CORES + 1 - core)
    near = i + 1 - 2 * zp
    zpair = (y, near, j)

    def plane(d):
        return (y, d, j)

    def at(yy, xx):
        return (yy, i, xx * CORES + core)

    def turn(v, o, size):
        return lax.rem(v + o, size)

    others = [(oy, ox) for oy in range(Y) for ox in range(X) if oy or ox]

    def has(d):
        return (d >= 0) & (d < n)

    HOPS = (1, 2, -1, -2)

    load_x = pltpu.make_async_copy(x_hbm, x_ref, x_sem)
    load_x.start()
    load_g = pltpu.make_async_copy(g_hbm, g_ref, g_sem)
    load_g.start()

    barrier = pltpu.get_barrier_semaphore()
    peers = len(others) + 1
    for step in HOPS:
        there = has(i + step)
        peers += there.astype(jnp.int32)

        @pl.when(there)
        def _():
            pl.semaphore_signal(barrier, inc=1, device_id=plane(i + step), device_id_type=MESH)

    pl.semaphore_signal(barrier, inc=1, device_id=partner, device_id_type=MESH)
    for oy, ox in others:
        pl.semaphore_signal(
            barrier, inc=1, device_id=at(turn(y, oy, Y), turn(x, ox, X)), device_id_type=MESH
        )

    def block_l(c, yy, xx):
        return c * PLANES * chips + yy * X + xx

    def block_f(c, yy, xx):
        return (c * PLANES + 1) * chips + xx * Y + yy

    def rows_at(first, size):
        return pl.ds(pl.multiple_of(first, B), size)

    def rows_of(b):
        return rows_at(b * B, B)

    mine, paired = block_l(core, y, x), block_f(core, y, x)

    def in_cols(d):
        return pl.ds(pl.multiple_of(((d % PLANES) * Y + y) * HU, HU), HU)

    def in_rows(s):
        return pl.ds(pl.multiple_of(s * Dr, Dr), Dr)

    def out_cols(cid):
        return pl.ds(pl.multiple_of(cid * W, W), W)

    pltpu.make_async_copy(wi_ref.at[:, in_cols(i)], wi.at[in_rows(i), :], wi_recv.at[i]).start()
    for h in range(parts):
        cid = i * parts + h
        pltpu.make_async_copy(
            wo_ref.at[in_cols(i), pl.ds(h * W, W)], wo.at[:, out_cols(cid)], wo_recv.at[cid]
        ).start()

    load_x.wait()
    load_g.wait()

    @pl.loop(0, B // 16)
    def _(r):
        rows = pl.ds(pl.multiple_of(r * 16, 16), 16)
        v = f32(x_ref[rows, :])
        scale = lax.rsqrt(jnp.mean(v * v, axis=-1, keepdims=True) + EPS)
        out_rows = pl.ds(pl.multiple_of(mine * B + r * 16, 16), 16)
        norm[out_rows, :] = (v * scale * g_ref[...]).astype(jnp.bfloat16)

    pl.semaphore_wait(barrier, peers)

    def send_in(step):
        d = i + step
        k = HOPS.index(step)

        @pl.when(has(d))
        def _():
            remote(wi_ref.at[:, in_cols(d)], wi.at[in_rows(i), :], wi_send.at[k], wi_recv.at[i], plane(d))

    def send_out(h, step):
        d = i + step
        k = HOPS.index(step)

        @pl.when(has(d))
        def _():
            cid = i * parts + h
            remote(
                wo_ref.at[in_cols(d), pl.ds(pl.multiple_of(h * W, W), W)], wo.at[:, out_cols(cid)],
                wo_send.at[h, k], wo_recv.at[cid], plane(d),
            )

    def both_ways(send):
        for sign in (1, -1):
            relayed = has(i + 3 * sign)

            @pl.when(relayed)
            def _():
                send(sign)
                send(2 * sign)

            @pl.when(jnp.logical_not(relayed))
            def _():
                send(2 * sign)
                send(sign)

    def onward(s):
        return jnp.where(s < i, i + 2, i - 2)

    def relays(s):
        return (s != i) & has(onward(s))

    def relay_in(s):
        @pl.when(relays(s))
        def _():
            ref = wi.at[in_rows(s), :]
            remote(ref, ref, wi_fwd.at[s], wi_recv.at[s], plane(onward(s)))

    def relay_out(cid):
        s = cid // parts

        @pl.when(relays(s))
        def _():
            ref = wo.at[:, out_cols(cid)]
            remote(ref, ref, wo_fwd.at[cid], wo_recv.at[cid], plane(onward(s)))

    count = [0]

    def send_block(b, device, into=None):
        into = b if into is None else into
        remote(
            norm.at[rows_of(b), :], norm.at[rows_of(into), :],
            tok_send.at[count[0]], tok_recv.at[into], device,
        )
        count[0] += 1

    send_block(mine, zpair, paired)
    both_ways(send_in)
    for oy, ox in others:
        send_block(mine, at(turn(y, oy, Y), turn(x, ox, X)))
    send_block(mine, partner)

    def arrived(b):
        done(norm.at[rows_of(b), :], tok_recv.at[b])

    arrived(paired)
    for oy, ox in others:
        send_block(paired, at(turn(y, oy, Y), turn(x, ox, X)))
    send_block(paired, partner)

    def in_arrived(s):
        done(wi.at[in_rows(s), :], wi_recv.at[s])
        relay_in(s)

    def source(k):
        if k == 0:
            return i
        if k == 1:
            return near
        pair = lax.rem(i // PLANES + k // PLANES, n // PLANES)
        e = k % PLANES
        return jnp.where(pair > i // PLANES, pair * PLANES + e, pair * PLANES + PLANES - 1 - e)

    inner = relays(near)

    def out_near(h):
        for step in (1, -1):
            pl.when(i + step == near)(functools.partial(send_out, h, step))

    def out_far(h):
        for step in (2, 1, -2, -1):
            pl.when(i + step != near)(functools.partial(send_out, h, step))

    def outer_out():
        for h in range(parts):
            out_near(h)
        for h in range(parts):
            out_far(h)

    pl.when(jnp.logical_not(inner))(outer_out)
    in_arrived(source(1))

    @pl.when(inner)
    def _():
        for h in range(parts):
            out_near(h)
        out_far(0)

    def near_out(h):
        cid = near * parts + h
        done(wo.at[:, out_cols(cid)], wo_recv.at[cid])

        @pl.when(inner)
        def _():
            relay_out(cid)
            pl.when(h + 1 < parts)(lambda: out_far(h + 1))

    for block in (block_l, block_f):
        for oy, ox in others:
            b = block(core, turn(y, Y - oy, Y), turn(x, X - ox, X))
            arrived(b)
            send_block(b, partner)
    for yy in range(Y):
        for xx in range(X):
            arrived(block_l(1 - core, yy, xx))
            arrived(block_f(1 - core, yy, xx))

    in_arrived(source(0))
    for k in range(2, n):
        in_arrived(source(k))

    near_out(0)

    TR = min(512, half)

    @pl.loop(0, R // TR)
    def _(r):
        rows = pl.ds(pl.multiple_of(r * TR, TR), TR)
        pre = jnp.dot(norm[rows, :], wi[...], preferred_element_type=jnp.float32)
        hid[rows, :] = jnp.square(jnp.maximum(pre, 0.0)).astype(jnp.bfloat16)

    for q in range(count[0]):
        done(norm.at[rows_of(0), :], tok_send.at[q])

    kept, given = core * half, (1 - core) * half

    ready = [(k, h) for k in (1, 0) for h in range(parts)]
    later = [(k, h) for k in range(2, n) for h in range(parts)]
    later.sort(key=lambda v: (v[1] + FAR_STEP * (v[0] - 2), v[0]))

    def chunk(t):
        code = jnp.int32(0)
        for q, (k, h) in enumerate(ready + later):
            code = jnp.where(t == q, k * parts + h, code)
        k, h = code // parts, code % parts
        pair = lax.rem(i // PLANES + k // PLANES, n // PLANES)
        e = k % PLANES
        far = jnp.where(pair > i // PLANES, pair * PLANES + e, pair * PLANES + PLANES - 1 - e)
        s = jnp.where(k == 0, near, jnp.where(k == 1, i, far))
        return s * parts + h

    TM = min(1024, half)

    def multiply(first, cols):
        for r in range(half // TM):
            rows = pl.ds(pl.multiple_of(first + r * TM, TM), TM)
            norm[rows, cols] = jnp.dot(
                hid[rows, :], wo[:, cols], preferred_element_type=jnp.float32
            ).astype(jnp.bfloat16)

    def fold(first, size, cols):
        rows = rows_at(kept + first, size)
        norm[rows, cols] = (f32(norm[rows, cols]) + f32(crecv[rows_at(first, size), cols])).astype(jnp.bfloat16)

    SL, SF = X * B, Y * B

    def part_sum(first, cols, landed, others_of, inside):
        v = f32(norm[rows_at(kept + first, B), cols]) + f32(crecv[rows_at(first, B), cols])
        for o in others_of:
            v += f32(landed[o, rows_at(inside, B), cols])
        return v

    def product(t):
        cid = chunk(t)
        cols = out_cols(cid)

        @pl.when(cid // parts != near)
        def _():
            done(wo.at[:, cols], wo_recv.at[cid])
            relay_out(cid)

        pl.when(t + 1 < parts)(lambda: near_out(t + 1))

        multiply(given, cols)
        remote(
            norm.at[rows_at(given, half), cols], crecv.at[:, cols], c_send, c_recv.at[cid], partner
        )
        multiply(kept, cols)

    def first_stage(t):
        cid = chunk(t)
        cols = out_cols(cid)
        done(crecv.at[:, cols], c_recv.at[cid])
        for o in range(1, X):
            xx = turn(x, o, X)
            fold(region + xx * SF, SF, cols)
            remote(
                norm.at[rows_at(kept + region + xx * SF, SF), cols], xf.at[x, :, cols],
                xf_send, xf_recv.at[cid * X + x], at(y, xx),
            )
        for o in range(1, Y):
            yy = turn(y, o, Y)
            fold(yy * SL, SL, cols)
            remote(
                norm.at[rows_at(kept + yy * SL, SL), cols], yl.at[y, :, cols],
                yl_send, yl_recv.at[cid * Y + y], at(yy, x),
            )

    def second_stage(t):
        cid = chunk(t)
        cols = out_cols(cid)
        xs = [turn(x, o, X) for o in range(1, X)]
        ys = [turn(y, o, Y) for o in range(1, Y)]
        for xx in xs:
            done(xf.at[xx, :, cols], xf_recv.at[cid * X + xx])
        for yy in ys:
            first = region + x * SF + yy * B
            norm[rows_at(kept + first, B), cols] = part_sum(first, cols, xf, xs, yy * B).astype(jnp.bfloat16)
            remote(
                norm.at[rows_at(kept + first, B), cols], yf.at[y, :, cols],
                yf_send, yf_recv.at[cid * Y + y], at(yy, x),
            )
        for yy in ys:
            done(yl.at[yy, :, cols], yl_recv.at[cid * Y + yy])
        for xx in xs:
            first = y * SL + xx * B
            norm[rows_at(kept + first, B), cols] = part_sum(first, cols, yl, ys, xx * B).astype(jnp.bfloat16)
            remote(
                norm.at[rows_at(kept + first, B), cols], xl.at[x, :, cols],
                xl_send, xl_recv.at[cid * X + x], at(y, xx),
            )
        own_f[:, cols] = part_sum(region + x * SF + y * B, cols, xf, xs, y * B)
        own_l[:, cols] = part_sum(y * SL + x * B, cols, yl, ys, x * B)

    def third_stage(t):
        cid = chunk(t)
        cols = out_cols(cid)
        v = own_f[:, cols]
        for o in range(1, Y):
            yy = turn(y, o, Y)
            done(yf.at[yy, :, cols], yf_recv.at[cid * Y + yy])
            v += f32(yf[yy, :, cols])
        zsend[:, cols] = v.astype(jnp.bfloat16)
        remote(zsend.at[:, cols], zrecv.at[:, cols], z_send, z_recv.at[cid], zpair)
        v = own_l[:, cols]
        for o in range(1, X):
            xx = turn(x, o, X)
            done(xl.at[xx, :, cols], xl_recv.at[cid * X + xx])
            v += f32(xl[xx, :, cols])
        own_l[:, cols] = v

    def finish(t):
        cid = chunk(t)
        cols = out_cols(cid)
        done(zrecv.at[:, cols], z_recv.at[cid])
        v = own_l[:, cols] + f32(zrecv[:, cols])
        out[:, cols] = (f32(x_ref[:, cols]) + v).astype(jnp.bfloat16)
        pltpu.make_async_copy(out.at[:, cols], o_hbm.at[:, cols], o_sem).start()

    def finish_far(t):
        pl.when(t >= len(ready))(lambda: finish(t))

    def finish_ready(t):
        pl.when(t < len(ready))(lambda: finish(t))

    LAG_5 = LAG_4 + parts
    stages = ((0, product), (LAG_1, first_stage), (LAG_2, second_stage), (LAG_3, third_stage),
              (LAG_4, finish_far), (LAG_5, finish_ready))

    @pl.loop(0, NC + LAG_4)
    def _(t):
        for lag, stage in stages:
            pl.when((t >= lag) & (t < NC + lag))(functools.partial(stage, t - lag))

    for k, step in enumerate(HOPS):
        @pl.when(has(i + step))
        def _():
            done(wi.at[in_rows(0), :], wi_send.at[k])
            for h in range(parts):
                done(wo.at[:, out_cols(0)], wo_send.at[h, k])

    for s in range(n):
        @pl.when(relays(s))
        def _():
            done(wi.at[in_rows(0), :], wi_fwd.at[s])
            for h in range(parts):
                done(wo.at[:, out_cols(0)], wo_fwd.at[s * parts + h])

    done(crecv, c_send)
    if Y > 1:
        done(yl.at[pl.ds(0, Y - 1)], yl_send)
        done(yf.at[pl.ds(0, Y - 1)], yf_send)
    if X > 1:
        done(xf.at[pl.ds(0, X - 1)], xf_send)
        done(xl.at[pl.ds(0, X - 1)], xl_send)
    done(zsend, z_send)
    pltpu.make_async_copy(out, o_hbm, o_sem).wait()


def solution(mesh):
    Y, n, T = mesh.shape["grp"], mesh.shape["fs"], mesh.shape["tp"]
    X = T // CORES
    chips = Y * X

    def local(tokens, norm_gain, w_in, w_out):
        B, D = tokens.shape
        HU = w_in.shape[1] // (PLANES * Y)
        parts = w_out.shape[1] // 128
        NC = n * parts
        R = CORES * chips * PLANES * B
        sends = 1 + 2 * chips + PLANES * (chips - 1)
        bf16 = jnp.bfloat16
        dma = pltpu.SemaphoreType.DMA
        hbm = pl.BlockSpec(memory_space=pl.ANY)
        return pl.pallas_call(
            functools.partial(kernel, Y, n, X, parts),
            out_shape=jax.ShapeDtypeStruct((B, D), bf16),
            in_specs=[hbm, hbm, hbm, hbm],
            out_specs=hbm,
            scratch_shapes=[
                pltpu.VMEM((R, D), bf16),
                pltpu.VMEM((D, HU), bf16),
                pltpu.VMEM((HU, D), bf16),
                pltpu.VMEM((R, HU), bf16),
                pltpu.VMEM((R // CORES, D), bf16),
                pltpu.VMEM((Y, X * B, D), bf16),
                pltpu.VMEM((X, Y * B, D), bf16),
                pltpu.VMEM((X, B, D), bf16),
                pltpu.VMEM((Y, B, D), bf16),
                pltpu.VMEM((B, D), jnp.float32),
                pltpu.VMEM((B, D), jnp.float32),
                pltpu.VMEM((B, D), bf16),
                pltpu.VMEM((B, D), bf16),
                pltpu.VMEM((B, D), bf16),
                pltpu.VMEM((1, D), jnp.float32),
                pltpu.VMEM((B, D), bf16),
                dma, dma, dma,
                dma((sends,)), dma((CORES * chips * PLANES,)),
                dma((4,)), dma((n,)),
                dma((parts, 4)), dma((NC,)),
                dma((n,)), dma((NC,)),
                dma, dma((NC,)),
                dma, dma((NC * Y,)),
                dma, dma((NC * X,)),
                dma, dma((NC * X,)),
                dma, dma((NC * Y,)),
                dma, dma((NC,)),
            ],
            compiler_params=pltpu.CompilerParams(
                collective_id=0, has_side_effects=True, vmem_limit_bytes=60 * 1024 * 1024
            ),
        )(tokens, norm_gain.reshape(1, D), w_in, w_out)

    in_specs = (P(("grp", "fs", "tp"), None), P(), P("fs", "tp"), P("tp", "fs"))
    out_specs = P(("grp", "fs", "tp"), None)
    return jax.shard_map(local, mesh=mesh, in_specs=in_specs, out_specs=out_specs, check_vma=False)
```

```python
import functools

import jax
import jax.numpy as jnp
from jax import lax
from jax.experimental import pallas as pl
from jax.experimental.pallas import tpu as pltpu
from jax.sharding import PartitionSpec as P

EPS = 1e-06
MESH = pl.DeviceIdType.MESH
CORES = 2
PLANES = 2
FAR_STEP = 0.0
LAG_1, LAG_2, LAG_3, LAG_4 = 1, 3, 5, 7


def remote(src, dst, send, recv, device):
    pltpu.make_async_remote_copy(
        src_ref=src, dst_ref=dst, send_sem=send, recv_sem=recv, device_id=device, device_id_type=MESH
    ).start()


def done(ref, sem):
    pltpu.make_async_copy(ref, ref, sem).wait()


def f32(value):
    return value.astype(jnp.float32)


def kernel(
    Y, n, X, parts, x_hbm, g_hbm, wi_ref, wo_ref, o_hbm,
    norm, wi, wo, hid, crecv, yl, xf, xl, yf, own_l, own_f, zsend, zrecv, x_ref, g_ref, out,
    x_sem, g_sem, o_sem, tok_send, tok_recv, wi_send, wi_recv, wo_send, wo_recv, wi_fwd, wo_fwd,
    c_send, c_recv, yl_send, yl_recv, xf_send, xf_recv, xl_send, xl_recv, yf_send, yf_recv, z_send, z_recv,
):
    y, i, j = lax.axis_index("grp"), lax.axis_index("fs"), lax.axis_index("tp")
    x, core, zp = j // CORES, j % CORES, i % PLANES
    chips = Y * X
    B, D = x_ref.shape
    HU = wi.shape[1]
    Dr, Dc = wi_ref.shape[0], wo_ref.shape[1]
    W = Dc // parts
    NC = n * parts
    R = norm.shape[0]
    half = R // CORES
    region = chips * B

    partner = (y, i, x * CORES + 1 - core)
    near = i + 1 - 2 * zp
    zpair = (y, near, j)

    def plane(d):
        return (y, d, j)

    def at(yy, xx):
        return (yy, i, xx * CORES + core)

    def turn(v, o, size):
        return lax.rem(v + o, size)

    others = [(oy, ox) for oy in range(Y) for ox in range(X) if oy or ox]

    def has(d):
        return (d >= 0) & (d < n)

    HOPS = (1, 2, -1, -2)


    barrier = pltpu.get_barrier_semaphore()
    peers = len(others) + 1
    for step in HOPS:
        there = has(i + step)
        peers += there.astype(jnp.int32)

        @pl.when(there)
        def _():
            pl.semaphore_signal(barrier, inc=1, device_id=plane(i + step), device_id_type=MESH)

    pl.semaphore_signal(barrier, inc=1, device_id=partner, device_id_type=MESH)
    for oy, ox in others:
        pl.semaphore_signal(
            barrier, inc=1, device_id=at(turn(y, oy, Y), turn(x, ox, X)), device_id_type=MESH
        )

    load_x = pltpu.make_async_copy(x_hbm, x_ref, x_sem)
    load_x.start()
    load_g = pltpu.make_async_copy(g_hbm, g_ref, g_sem)
    load_g.start()

    def block_l(c, yy, xx):
        return c * PLANES * chips + yy * X + xx

    def block_f(c, yy, xx):
        return (c * PLANES + 1) * chips + xx * Y + yy

    def rows_at(first, size):
        return pl.ds(pl.multiple_of(first, B), size)

    def rows_of(b):
        return rows_at(b * B, B)

    mine, paired = block_l(core, y, x), block_f(core, y, x)

    def in_cols(d):
        return pl.ds(pl.multiple_of(((d % PLANES) * Y + y) * HU, HU), HU)

    def in_rows(s):
        return pl.ds(pl.multiple_of(s * Dr, Dr), Dr)

    def out_cols(cid):
        return pl.ds(pl.multiple_of(cid * W, W), W)

    pltpu.make_async_copy(wi_ref.at[:, in_cols(i)], wi.at[in_rows(i), :], wi_recv.at[i]).start()
    for h in range(parts):
        cid = i * parts + h
        pltpu.make_async_copy(
            wo_ref.at[in_cols(i), pl.ds(h * W, W)], wo.at[:, out_cols(cid)], wo_recv.at[cid]
        ).start()

    load_x.wait()
    load_g.wait()

    @pl.loop(0, B // 16)
    def _(r):
        rows = pl.ds(pl.multiple_of(r * 16, 16), 16)
        v = f32(x_ref[rows, :])
        scale = lax.rsqrt(jnp.mean(v * v, axis=-1, keepdims=True) + EPS)
        out_rows = pl.ds(pl.multiple_of(mine * B + r * 16, 16), 16)
        norm[out_rows, :] = (v * scale * g_ref[...]).astype(jnp.bfloat16)

    pl.semaphore_wait(barrier, peers)

    def send_in(step):
        d = i + step
        k = HOPS.index(step)

        @pl.when(has(d))
        def _():
            remote(wi_ref.at[:, in_cols(d)], wi.at[in_rows(i), :], wi_send.at[k], wi_recv.at[i], plane(d))

    def send_out(h, step):
        d = i + step
        k = HOPS.index(step)

        @pl.when(has(d))
        def _():
            cid = i * parts + h
            remote(
                wo_ref.at[in_cols(d), pl.ds(pl.multiple_of(h * W, W), W)], wo.at[:, out_cols(cid)],
                wo_send.at[h, k], wo_recv.at[cid], plane(d),
            )

    def both_ways(send):
        for sign in (1, -1):
            relayed = has(i + 3 * sign)

            @pl.when(relayed)
            def _():
                send(sign)
                send(2 * sign)

            @pl.when(jnp.logical_not(relayed))
            def _():
                send(2 * sign)
                send(sign)

    def onward(s):
        return jnp.where(s < i, i + 2, i - 2)

    def relays(s):
        return (s != i) & has(onward(s))

    def relay_in(s):
        @pl.when(relays(s))
        def _():
            ref = wi.at[in_rows(s), :]
            remote(ref, ref, wi_fwd.at[s], wi_recv.at[s], plane(onward(s)))

    def relay_out(cid):
        s = cid // parts

        @pl.when(relays(s))
        def _():
            ref = wo.at[:, out_cols(cid)]
            remote(ref, ref, wo_fwd.at[cid], wo_recv.at[cid], plane(onward(s)))

    count = [0]

    def send_block(b, device, into=None):
        into = b if into is None else into
        remote(
            norm.at[rows_of(b), :], norm.at[rows_of(into), :],
            tok_send.at[count[0]], tok_recv.at[into], device,
        )
        count[0] += 1

    send_block(mine, zpair, paired)
    both_ways(send_in)
    for oy, ox in others:
        send_block(mine, at(turn(y, oy, Y), turn(x, ox, X)))
    send_block(mine, partner)

    def arrived(b):
        done(norm.at[rows_of(b), :], tok_recv.at[b])

    arrived(paired)
    for oy, ox in others:
        send_block(paired, at(turn(y, oy, Y), turn(x, ox, X)))
    send_block(paired, partner)

    def in_arrived(s):
        done(wi.at[in_rows(s), :], wi_recv.at[s])
        relay_in(s)

    def source(k):
        if k == 0:
            return i
        if k == 1:
            return near
        pair = lax.rem(i // PLANES + k // PLANES, n // PLANES)
        e = k % PLANES
        return jnp.where(pair > i // PLANES, pair * PLANES + e, pair * PLANES + PLANES - 1 - e)

    inner = relays(near)

    def out_near(h):
        for step in (1, -1):
            pl.when(i + step == near)(functools.partial(send_out, h, step))

    def out_far(h):
        for step in (2, 1, -2, -1):
            pl.when(i + step != near)(functools.partial(send_out, h, step))

    def outer_out():
        for h in range(parts):
            out_near(h)
        for h in range(parts):
            out_far(h)

    pl.when(jnp.logical_not(inner))(outer_out)
    in_arrived(source(1))

    @pl.when(inner)
    def _():
        for h in range(parts):
            out_near(h)
        out_far(0)

    def near_out(h):
        cid = near * parts + h
        done(wo.at[:, out_cols(cid)], wo_recv.at[cid])

        @pl.when(inner)
        def _():
            relay_out(cid)
            pl.when(h + 1 < parts)(lambda: out_far(h + 1))

    for block in (block_l, block_f):
        for oy, ox in others:
            b = block(core, turn(y, Y - oy, Y), turn(x, X - ox, X))
            arrived(b)
            send_block(b, partner)
    for yy in range(Y):
        for xx in range(X):
            arrived(block_l(1 - core, yy, xx))
            arrived(block_f(1 - core, yy, xx))

    in_arrived(source(0))
    for k in range(2, n):
        in_arrived(source(k))

    near_out(0)

    TR = min(512, half)

    @pl.loop(0, R // TR)
    def _(r):
        rows = pl.ds(pl.multiple_of(r * TR, TR), TR)
        pre = jnp.dot(norm[rows, :], wi[...], preferred_element_type=jnp.float32)
        hid[rows, :] = jnp.square(jnp.maximum(pre, 0.0)).astype(jnp.bfloat16)

    for q in range(count[0]):
        done(norm.at[rows_of(0), :], tok_send.at[q])

    kept, given = core * half, (1 - core) * half

    ready = [(k, h) for k in (1, 0) for h in range(parts)]
    later = [(k, h) for k in range(2, n) for h in range(parts)]
    later.sort(key=lambda v: (v[1] + FAR_STEP * (v[0] - 2), v[0]))

    def chunk(t):
        code = jnp.int32(0)
        for q, (k, h) in enumerate(ready + later):
            code = jnp.where(t == q, k * parts + h, code)
        k, h = code // parts, code % parts
        pair = lax.rem(i // PLANES + k // PLANES, n // PLANES)
        e = k % PLANES
        far = jnp.where(pair > i // PLANES, pair * PLANES + e, pair * PLANES + PLANES - 1 - e)
        s = jnp.where(k == 0, near, jnp.where(k == 1, i, far))
        return s * parts + h

    TM = min(1024, half)

    def multiply(first, cols):
        for r in range(half // TM):
            rows = pl.ds(pl.multiple_of(first + r * TM, TM), TM)
            norm[rows, cols] = jnp.dot(
                hid[rows, :], wo[:, cols], preferred_element_type=jnp.float32
            ).astype(jnp.bfloat16)

    def fold(first, size, cols):
        rows = rows_at(kept + first, size)
        norm[rows, cols] = (f32(norm[rows, cols]) + f32(crecv[rows_at(first, size), cols])).astype(jnp.bfloat16)

    SL, SF = X * B, Y * B

    def part_sum(first, cols, landed, others_of, inside):
        v = f32(norm[rows_at(kept + first, B), cols]) + f32(crecv[rows_at(first, B), cols])
        for o in others_of:
            v += f32(landed[o, rows_at(inside, B), cols])
        return v

    def product(t):
        cid = chunk(t)
        cols = out_cols(cid)

        @pl.when(cid // parts != near)
        def _():
            done(wo.at[:, cols], wo_recv.at[cid])
            relay_out(cid)

        pl.when(t + 1 < parts)(lambda: near_out(t + 1))

        multiply(given, cols)
        remote(
            norm.at[rows_at(given, half), cols], crecv.at[:, cols], c_send, c_recv.at[cid], partner
        )
        multiply(kept, cols)

    def first_stage(t):
        cid = chunk(t)
        cols = out_cols(cid)
        done(crecv.at[:, cols], c_recv.at[cid])
        for o in range(1, X):
            xx = turn(x, o, X)
            fold(region + xx * SF, SF, cols)
            remote(
                norm.at[rows_at(kept + region + xx * SF, SF), cols], xf.at[x, :, cols],
                xf_send, xf_recv.at[cid * X + x], at(y, xx),
            )
        for o in range(1, Y):
            yy = turn(y, o, Y)
            fold(yy * SL, SL, cols)
            remote(
                norm.at[rows_at(kept + yy * SL, SL), cols], yl.at[y, :, cols],
                yl_send, yl_recv.at[cid * Y + y], at(yy, x),
            )

    def second_stage(t):
        cid = chunk(t)
        cols = out_cols(cid)
        xs = [turn(x, o, X) for o in range(1, X)]
        ys = [turn(y, o, Y) for o in range(1, Y)]
        for xx in xs:
            done(xf.at[xx, :, cols], xf_recv.at[cid * X + xx])
        for yy in ys:
            first = region + x * SF + yy * B
            norm[rows_at(kept + first, B), cols] = part_sum(first, cols, xf, xs, yy * B).astype(jnp.bfloat16)
            remote(
                norm.at[rows_at(kept + first, B), cols], yf.at[y, :, cols],
                yf_send, yf_recv.at[cid * Y + y], at(yy, x),
            )
        for yy in ys:
            done(yl.at[yy, :, cols], yl_recv.at[cid * Y + yy])
        for xx in xs:
            first = y * SL + xx * B
            norm[rows_at(kept + first, B), cols] = part_sum(first, cols, yl, ys, xx * B).astype(jnp.bfloat16)
            remote(
                norm.at[rows_at(kept + first, B), cols], xl.at[x, :, cols],
                xl_send, xl_recv.at[cid * X + x], at(y, xx),
            )
        own_f[:, cols] = part_sum(region + x * SF + y * B, cols, xf, xs, y * B)
        own_l[:, cols] = part_sum(y * SL + x * B, cols, yl, ys, x * B)

    def third_stage(t):
        cid = chunk(t)
        cols = out_cols(cid)
        v = own_f[:, cols]
        for o in range(1, Y):
            yy = turn(y, o, Y)
            done(yf.at[yy, :, cols], yf_recv.at[cid * Y + yy])
            v += f32(yf[yy, :, cols])
        zsend[:, cols] = v.astype(jnp.bfloat16)
        remote(zsend.at[:, cols], zrecv.at[:, cols], z_send, z_recv.at[cid], zpair)
        v = own_l[:, cols]
        for o in range(1, X):
            xx = turn(x, o, X)
            done(xl.at[xx, :, cols], xl_recv.at[cid * X + xx])
            v += f32(xl[xx, :, cols])
        own_l[:, cols] = v

    def finish(t):
        cid = chunk(t)
        cols = out_cols(cid)
        done(zrecv.at[:, cols], z_recv.at[cid])
        v = own_l[:, cols] + f32(zrecv[:, cols])
        out[:, cols] = (f32(x_ref[:, cols]) + v).astype(jnp.bfloat16)
        pltpu.make_async_copy(out.at[:, cols], o_hbm.at[:, cols], o_sem).start()

    def finish_far(t):
        pl.when(t >= len(ready))(lambda: finish(t))

    def finish_ready(t):
        pl.when(t < len(ready))(lambda: finish(t))

    LAG_5 = LAG_4 + parts
    stages = ((0, product), (LAG_1, first_stage), (LAG_2, second_stage), (LAG_3, third_stage),
              (LAG_4, finish_far), (LAG_5, finish_ready))

    @pl.loop(0, NC + LAG_4)
    def _(t):
        for lag, stage in stages:
            pl.when((t >= lag) & (t < NC + lag))(functools.partial(stage, t - lag))

    for k, step in enumerate(HOPS):
        @pl.when(has(i + step))
        def _():
            done(wi.at[in_rows(0), :], wi_send.at[k])
            for h in range(parts):
                done(wo.at[:, out_cols(0)], wo_send.at[h, k])

    for s in range(n):
        @pl.when(relays(s))
        def _():
            done(wi.at[in_rows(0), :], wi_fwd.at[s])
            for h in range(parts):
                done(wo.at[:, out_cols(0)], wo_fwd.at[s * parts + h])

    done(crecv, c_send)
    if Y > 1:
        done(yl.at[pl.ds(0, Y - 1)], yl_send)
        done(yf.at[pl.ds(0, Y - 1)], yf_send)
    if X > 1:
        done(xf.at[pl.ds(0, X - 1)], xf_send)
        done(xl.at[pl.ds(0, X - 1)], xl_send)
    done(zsend, z_send)
    pltpu.make_async_copy(out, o_hbm, o_sem).wait()


def solution(mesh):
    Y, n, T = mesh.shape["grp"], mesh.shape["fs"], mesh.shape["tp"]
    X = T // CORES
    chips = Y * X

    def local(tokens, norm_gain, w_in, w_out):
        B, D = tokens.shape
        HU = w_in.shape[1] // (PLANES * Y)
        parts = w_out.shape[1] // 128
        NC = n * parts
        R = CORES * chips * PLANES * B
        sends = 1 + 2 * chips + PLANES * (chips - 1)
        bf16 = jnp.bfloat16
        dma = pltpu.SemaphoreType.DMA
        hbm = pl.BlockSpec(memory_space=pl.ANY)
        return pl.pallas_call(
            functools.partial(kernel, Y, n, X, parts),
            out_shape=jax.ShapeDtypeStruct((B, D), bf16),
            in_specs=[hbm, hbm, hbm, hbm],
            out_specs=hbm,
            scratch_shapes=[
                pltpu.VMEM((R, D), bf16),
                pltpu.VMEM((D, HU), bf16),
                pltpu.VMEM((HU, D), bf16),
                pltpu.VMEM((R, HU), bf16),
                pltpu.VMEM((R // CORES, D), bf16),
                pltpu.VMEM((Y, X * B, D), bf16),
                pltpu.VMEM((X, Y * B, D), bf16),
                pltpu.VMEM((X, B, D), bf16),
                pltpu.VMEM((Y, B, D), bf16),
                pltpu.VMEM((B, D), jnp.float32),
                pltpu.VMEM((B, D), jnp.float32),
                pltpu.VMEM((B, D), bf16),
                pltpu.VMEM((B, D), bf16),
                pltpu.VMEM((B, D), bf16),
                pltpu.VMEM((1, D), jnp.float32),
                pltpu.VMEM((B, D), bf16),
                dma, dma, dma,
                dma((sends,)), dma((CORES * chips * PLANES,)),
                dma((4,)), dma((n,)),
                dma((parts, 4)), dma((NC,)),
                dma((n,)), dma((NC,)),
                dma, dma((NC,)),
                dma, dma((NC * Y,)),
                dma, dma((NC * X,)),
                dma, dma((NC * X,)),
                dma, dma((NC * Y,)),
                dma, dma((NC,)),
            ],
            compiler_params=pltpu.CompilerParams(
                collective_id=0, has_side_effects=True, vmem_limit_bytes=60 * 1024 * 1024
            ),
        )(tokens, norm_gain.reshape(1, D), w_in, w_out)

    in_specs = (P(("grp", "fs", "tp"), None), P(), P("fs", "tp"), P("tp", "fs"))
    out_specs = P(("grp", "fs", "tp"), None)
    return jax.shard_map(local, mesh=mesh, in_specs=in_specs, out_specs=out_specs, check_vma=False)
```
